32 devices in a mesh: grp: 2 (over x), sp: 4 (over y, core), tp: 4 (over z).
Axes of the slice: x: 2, y: 2, z: 4, core: 2. Of those that a mesh axis runs over, the one named last changes fastest.
Arguments:
- tokens_in: bfloat16 [2048, 2048], P(('grp', 'sp'), 'tp'), parts along dimension 0, may hold values from -8 to 8
- out_gate: bfloat16 [3, 2048, 2048], P(None, 'sp', 'tp'), may hold values from -0.125 to 0.125
- in_gate: bfloat16 [3, 2048, 2048], P(None, 'sp', 'tp'), may hold values from -0.125 to 0.125
- value_proj: bfloat16 [3, 2048, 2048], P(None, 'sp', 'tp'), may hold values from -0.125 to 0.125
- mix_proj: bfloat16 [3, 2048, 2048], P(None, 'sp', 'tp'), may hold values from -0.125 to 0.125
- conv_taps: float32 [3, 3, 2048], P(None, None, 'tp'), may hold values from -3.5 to 3.5
- norm_gains: float32 [3, 2048], P(None, 'tp'), may hold values from 0.1 to 1.9
- final_gain: float32 [2048], P('tp'), may hold values from 0.1 to 1.9
Outputs:
- normed_out: bfloat16 [2048, 2048], P(('grp', 'sp'), 'tp'), parts along dimension 0
The draws below stay inside these ranges and needn't reach their ends.
There are 2 independent parts, one for each index of `grp`. The reference program is written for one: setup_inputs(seed, part) draws one part's arguments, and reference() takes and returns one part's arrays. A program takes and returns all parts, laid end to end along the dimension named above; an argument that names none is the same for every part. Nothing has to cross between parts.
All inputs are finite; a program needn't handle non-finite values.
Results may differ from the reference program's by a relative error of at most 0.025.
Values may be sent and summed in bfloat16 or wider, within the bound.
A program may use at most 64 MiB of HBM per device.

```python
import jax
import jax.numpy as jnp
from jax import lax

D = 2048
TAPS = 3
LAYERS = 3
TOKENS = 1024


def draw_tokens_in(key, part):
    keys = jax.random.split(jax.random.fold_in(key, 11), 2)
    ramp = jnp.exp(jnp.linspace(jnp.log(0.5), jnp.log(2.0), D)).astype(jnp.float32)
    rough = jnp.exp(jax.random.uniform(keys[1], (D,), jnp.float32, -0.35, 0.35))
    values = jax.random.normal(keys[0], (TOKENS, D), jnp.float32) * ramp * rough
    return jnp.clip(values, -8.0, 8.0).astype(jnp.bfloat16)


def block_levels(own_key, shape, shards, smallest, high):
    loudness, own = 1.0, jax.random.fold_in(own_key, 6)
    for axis_at, blocks in shards:
        heights = jnp.exp(jax.random.uniform(jax.random.fold_in(own, axis_at), (blocks,), jnp.float32, smallest / len(shards), high / len(shards)))
        loudness = loudness * jnp.repeat(heights, shape[axis_at] // blocks).reshape([-1 if axis == axis_at else 1 for axis in range(len(shape))])
    return loudness


def normal_values(rng, shape, width, most, cuts=(), held_as=jnp.bfloat16):
    entries = jax.random.normal(rng, shape, jnp.float32) * width
    if len(cuts) > 0:
        entries = block_levels(rng, shape, cuts, -0.22, 0.18) * entries
    return jnp.clip(entries, min=-most, max=most).astype(held_as)


def setup_inputs(seed: int = 0, part: int = 0) -> dict:
    arg_keys = jax.random.split(jax.random.key(seed), 9)
    own_keys = jax.random.split(jax.random.fold_in(arg_keys[8], part), 9)
    tokens_in = draw_tokens_in(jax.random.fold_in(jax.random.fold_in(arg_keys[8], part), 71), part)
    out_gate = normal_values(arg_keys[1], (LAYERS, D, D), D ** -0.5, 0.125, ((1, 4), (2, 4)))
    in_gate = normal_values(arg_keys[2], (LAYERS, D, D), D ** -0.5, 0.125, ((1, 4), (2, 4)))
    value_proj = normal_values(arg_keys[3], (LAYERS, D, D), D ** -0.5, 0.125, ((1, 4), (2, 4)))
    mix_proj = normal_values(arg_keys[4], (LAYERS, D, D), D ** -0.5, 0.125, ((1, 4), (2, 4)))
    conv_taps = normal_values(arg_keys[5], (LAYERS, TAPS, D), TAPS ** -0.5, 3.5, ((2, 4),), jnp.float32)
    norm_gains = jnp.clip(1.0 + 0.18 * jax.random.normal(arg_keys[6], (LAYERS, D), jnp.float32), 0.1, 1.9)
    final_gain = jnp.clip(1.0 + 0.18 * jax.random.normal(arg_keys[7], (D,), jnp.float32), 0.1, 1.9)
    return {"tokens_in": tokens_in, "out_gate": out_gate, "in_gate": in_gate, "value_proj": value_proj, "mix_proj": mix_proj, "conv_taps": conv_taps, "norm_gains": norm_gains, "final_gain": final_gain}


epsilon = 1e-06

def reference(tokens_in, out_gate, in_gate, value_proj, mix_proj, conv_taps, norm_gains, final_gain):
    stream = tokens_in.astype(jnp.float32)
    reach = TAPS - 1
    for layer_index in range(LAYERS):
        scale = lax.rsqrt(lax.optimization_barrier(jnp.sum(stream * stream, axis=1, keepdims=True)) / D + epsilon)
        normed = (stream * norm_gains[layer_index]).astype(jnp.bfloat16)
        out_gates = (jnp.dot(normed, out_gate[layer_index], preferred_element_type=jnp.float32) * scale).astype(jnp.bfloat16)
        in_gates = (jnp.dot(normed, in_gate[layer_index], preferred_element_type=jnp.float32) * scale).astype(jnp.bfloat16)
        values = (jnp.dot(normed, value_proj[layer_index], preferred_element_type=jnp.float32) * scale).astype(jnp.bfloat16)
        product_v = (in_gates.astype(jnp.float32) * values.astype(jnp.float32)).astype(jnp.bfloat16)
        padded = jnp.concatenate([jnp.zeros((reach, D), jnp.bfloat16), product_v], axis=0)
        convolved = jnp.zeros((TOKENS, D), jnp.float32)
        for tap_index in range(TAPS):
            convolved = convolved + padded[tap_index:tap_index + TOKENS].astype(jnp.float32) * conv_taps[layer_index, tap_index]
        gated = (out_gates.astype(jnp.float32) * convolved).astype(jnp.bfloat16)
        stream = stream + jnp.dot(gated, mix_proj[layer_index], preferred_element_type=jnp.float32)
    scale = lax.rsqrt(lax.optimization_barrier(jnp.sum(stream * stream, axis=1, keepdims=True)) / D + epsilon)
    return (stream * scale * final_gain).astype(jnp.bfloat16)
```

```python
import functools

import jax
import jax.numpy as jnp
from jax import lax
from jax.experimental import pallas as pl
from jax.experimental.pallas import tpu as pltpu
from jax.sharding import PartitionSpec as P

epsilon = 1e-06
MESH = pl.DeviceIdType.MESH
HALO = 16
CORES = 2
VMEM_LIMIT = 67043328


def kernel(
    sizes,
    tokens,
    in_gate,
    value_proj,
    out_gate,
    mix_proj,
    taps,
    gains,
    final_gain,
    out,
    weights,
    gather_a,
    gather_b,
    squares_a,
    squares_b,
    stream,
    products,
    halo,
    own_sem,
    halo_sems,
    pair_send,
    pair_recv,
    row_send,
    row_recv,
    cross_send,
    cross_recv,
    relay_send,
    relay_recv,
    act_send,
    act_recv,
    act_fwd,
    sq_send,
    sq_recv,
):
    groups, sp_count, tp_count, layers, tap_count = sizes
    rows, width = tokens.shape
    depth = in_gate.shape[1]
    full = depth * sp_count
    part = depth // groups
    chips = sp_count // CORES
    mats = (in_gate, value_proj, out_gate, mix_proj)
    g = lax.axis_index("grp")
    s = lax.axis_index("sp")
    t = lax.axis_index("tp")
    y, core = s // CORES, s % CORES
    partner = y * CORES + (1 - core)
    half = rows // 2
    counts = (HALO + half, rows - half)
    starts = (0, HALO + half)
    gathers = (gather_a, gather_b)
    squares = (squares_a, squares_b)

    def remote(src, dst, send, recv, where):
        return pltpu.make_async_remote_copy(
            src_ref=src, dst_ref=dst, send_sem=send, recv_sem=recv, device_id=where, device_id_type=MESH
        )

    barrier = pltpu.get_barrier_semaphore()
    for axis, me, count in (("tp", t, tp_count), ("sp", s, sp_count), ("grp", g, groups)):
        for by in range(1, count):
            pl.semaphore_signal(barrier, inc=1, device_id={axis: lax.rem(me + by, count)}, device_id_type=MESH)

    for c in range(2):
        for index in range(layers + 1):
            squares[c][index, t] = jnp.zeros(squares[c].shape[2:], jnp.float32)
    products[0:8, :] = jnp.zeros((8, width), jnp.float32)

    @pl.when(s == 0)
    def _():
        halo[...] = jnp.zeros_like(halo)

    pl.semaphore_wait(barrier, tp_count - 1 + sp_count - 1 + groups - 1)

    def block(index, owner, piece):
        return weights.at[index, pl.ds(pl.multiple_of(owner * depth + piece * part, 8), part), :]

    def whole_block(index, owner):
        return weights.at[index, pl.ds(pl.multiple_of(owner * depth, 8), depth), :]

    def own_copy(layer, m):
        index = layer * 4 + m
        return pltpu.make_async_copy(mats[m].at[layer], whole_block(index, s), own_sem.at[index])

    def pair_copy(layer, m, owner):
        index = layer * 4 + m
        return remote(
            mats[m].at[layer], whole_block(index, owner), pair_send.at[index], pair_recv.at[index], {"sp": partner}
        )

    def row_copy(layer, m, by):
        index = layer * 4 + m
        to = lax.rem(y + by, chips) * CORES + core
        return remote(
            mats[m].at[layer, pl.ds(pl.multiple_of(g * part, 8), part), :],
            block(index, s, g),
            row_send.at[index, by - 1],
            row_recv.at[index, by - 1],
            {"sp": to},
        )

    def source(by):
        return lax.rem(y + chips - by, chips) * CORES + core

    def row_arrival(index, by):
        ref = block(index, source(by), g)
        return remote(ref, ref, row_send.at[index, by - 1], row_recv.at[index, by - 1], {"sp": partner})

    def cross_copy(index, by, step):
        ref = block(index, source(by), g)
        return remote(
            ref,
            ref,
            cross_send.at[index, by - 1, step - 1],
            cross_recv.at[index, by - 1, step - 1],
            {"grp": lax.rem(g + step, groups)},
        )

    def cross_arrival(index, by, step):
        ref = block(index, source(by), lax.rem(g + groups - step, groups))
        return remote(
            ref,
            ref,
            cross_send.at[index, by - 1, step - 1],
            cross_recv.at[index, by - 1, step - 1],
            {"grp": lax.rem(g + step, groups)},
        )

    def relay_copy(index, by, step, of_partner=False):
        owner = source(by)
        if of_partner:
            owner = lax.rem(y + chips - by, chips) * CORES + (1 - core)
        ref = block(index, owner, lax.rem(g + groups - step, groups))
        return remote(
            ref, ref, relay_send.at[index, by - 1, step], relay_recv.at[index, by - 1, step], {"sp": partner}
        )

    def serve_rows(index):
        for by in range(1, chips):
            row_arrival(index, by).wait_recv()
            for step in range(1, groups):
                cross_copy(index, by, step).start()
            relay_copy(index, by, 0).start()

    def serve_cross(index):
        for by in range(1, chips):
            for step in range(1, groups):
                cross_arrival(index, by, step).wait_recv()
                relay_copy(index, by, step).start()

    def weights_ready(layer, m):
        index = layer * 4 + m
        own_copy(layer, m).wait()
        pair_copy(layer, m, partner).wait_recv()
        for by in range(1, chips):
            for step in range(groups):
                relay_copy(index, by, step, True).wait_recv()

    def columns(owner):
        return pl.ds(pl.multiple_of(owner * width, 128), width)

    def act_copy(c, stage, owner, to, send):
        ref = gathers[c].at[stage, :, columns(owner)]
        return remote(ref, ref, send, act_recv.at[c, stage, owner], {"tp": to})

    OFFSETS = (2, -2, 1, -1)

    def inside(index):
        return (index >= 0) & (index < tp_count)

    def act_each(c, stage, what):
        for j, by in enumerate(OFFSETS):
            if abs(by) < tp_count:

                @pl.when(inside(t + by))
                def _(j=j, by=by):
                    what(act_copy(c, stage, t, t + by, act_send.at[c, stage, j]))

    def act_forwards(c, stage, start):
        for k in range(1, (tp_count + 1) // 2):
            for side, sign in enumerate((1, -1)):
                origin = t - 2 * k * sign

                @pl.when(inside(origin) & inside(t + sign))
                def _(k=k, side=side, sign=sign, origin=origin):
                    if start:
                        act_copy(c, stage, origin, t + sign, act_fwd.at[c, stage, k - 1, side, 0]).wait_recv()
                    for far in (2, 1):

                        @pl.when(inside(t + sign * far))
                        def _(far=far):
                            copy = act_copy(
                                c, stage, origin, t + sign * far, act_fwd.at[c, stage, k - 1, side, far - 1]
                            )
                            if start:
                                copy.start()
                            else:
                                copy.wait_send()

    def act_finish(c, stage):
        for owner in range(tp_count):
            right = (owner < t) & (lax.rem(t - owner + tp_count * 2, 2) == 0) & (t + 1 < tp_count)
            left = (owner > t) & (lax.rem(owner - t + tp_count * 2, 2) == 0) & (t >= 1)

            @pl.when((owner != t) & jnp.logical_not(right | left))
            def _(owner=owner):
                act_copy(c, stage, owner, t, act_send.at[c, stage, 0]).wait_recv()

    def sq_copy(c, index, by):
        ref = squares[c].at[index, t]
        return remote(
            ref,
            ref,
            sq_send.at[c, index, by - 1],
            sq_recv.at[c, index, by - 1],
            {"tp": lax.rem(t + by, tp_count)},
        )

    def span(c):
        return pl.ds(starts[c], counts[c])

    def send_normed(c, layer):
        now = stream[span(c), :]
        gathers[c][2 * layer, :, columns(t)] = (now * gains[pl.ds(layer, 1), :]).astype(jnp.bfloat16)
        act_each(c, 2 * layer, lambda copy: copy.start())

    def send_squares(c, index):
        now = stream[span(c), :]
        sums = lax.dot_general(
            jnp.ones((8, width), jnp.float32),
            now * now,
            (((1,), (1,)), ((), ())),
            precision=lax.Precision.HIGHEST,
            preferred_element_type=jnp.float32,
        )
        squares[c][index, t, :, 0 : counts[c]] = sums
        for by in range(1, tp_count):
            sq_copy(c, index, by).start()

    def row_scale(c, index):
        for by in range(1, tp_count):
            sq_copy(c, index, by).wait_recv()
        total = squares[c][index, 0]
        for owner in range(1, tp_count):
            total = total + squares[c][index, owner]
        scale = lax.rsqrt(total / full + epsilon)
        return jnp.transpose(scale)[0 : counts[c], 0:1]

    @pl.when(s + 1 < sp_count)
    def _():
        remote(
            tokens.at[pl.ds(rows - HALO, HALO), :], halo, halo_sems.at[0], halo_sems.at[1], {"sp": s + 1}
        ).start()

    for layer in range(1):
        for m in range(3):
            for by in range(1, chips):
                row_copy(layer, m, by).start()
            pair_copy(layer, m, s).start()
            own_copy(layer, m).start()

    stream[HALO:, :] = tokens[...].astype(jnp.float32)
    send_normed(1, 0)

    @pl.when(s > 0)
    def _():
        remote(halo, halo, halo_sems.at[0], halo_sems.at[1], {"sp": partner}).wait_recv()

    stream[0:HALO, :] = halo[...].astype(jnp.float32)
    send_normed(0, 0)
    send_squares(0, 0)
    send_squares(1, 0)

    for index in range(3, layers * 4):
        layer, m = divmod(index, 4)
        for by in range(1, chips):
            row_copy(layer, m, by).start()
        pair_copy(layer, m, s).start()
        own_copy(layer, m).start()

    act_forwards(0, 0, True)
    act_forwards(1, 0, True)
    serve_rows(0)
    serve_rows(1)
    serve_cross(0)
    serve_rows(2)
    serve_cross(1)

    def project(c, layer):
        stage = 2 * layer
        act_finish(c, stage)
        if c == 0:
            for m in range(3):
                weights_ready(layer, m)
        seen = gathers[c][stage]
        scale = row_scale(c, layer)
        ins, values, outs = [
            (jnp.dot(seen, weights[layer * 4 + m], preferred_element_type=jnp.float32) * scale).astype(jnp.bfloat16)
            for m in range(3)
        ]
        made = (ins.astype(jnp.float32) * values.astype(jnp.float32)).astype(jnp.bfloat16)
        products[pl.ds(8 + starts[c], counts[c]), :] = made.astype(jnp.float32)
        total = None
        for k in range(tap_count):
            term = products[pl.ds(8 + starts[c] - (tap_count - 1) + k, counts[c]), :] * taps[layer, pl.ds(k, 1), :]
            total = term if total is None else total + term
        gathers[c][stage + 1, :, columns(t)] = (outs.astype(jnp.float32) * total).astype(jnp.bfloat16)
        act_each(c, stage + 1, lambda copy: copy.start())

    def mix(c, layer):
        stage = 2 * layer + 1
        act_finish(c, stage)
        if c == 0:
            weights_ready(layer, 3)
        stream[span(c), :] += jnp.dot(
            gathers[c][stage], weights[layer * 4 + 3], preferred_element_type=jnp.float32
        )

        @pl.when(layer + 1 < layers)
        def _():
            send_normed(c, layer + 1)

        send_squares(c, layer + 1)

    def one_layer(layer, carry):
        index = 4 * layer
        more = layer + 1 < layers

        @pl.when(layer > 0)
        def _():
            act_forwards(0, 2 * layer, True)

        serve_cross(index + 2)
        project(0, layer)

        @pl.when(layer > 0)
        def _():
            act_forwards(1, 2 * layer, True)

        project(1, layer)
        serve_rows(index + 3)
        act_forwards(0, 2 * layer + 1, True)
        serve_cross(index + 3)
        mix(0, layer)
        act_forwards(1, 2 * layer + 1, True)

        @pl.when(more)
        def _():
            serve_rows(index + 4)
            serve_rows(index + 5)
            serve_cross(index + 4)

        mix(1, layer)

        @pl.when(more)
        def _():
            serve_rows(index + 6)
            serve_cross(index + 5)

        return carry

    lax.fori_loop(0, layers, one_layer, 0)

    for c in range(2):
        first = HALO if c == 0 else 0
        scale = row_scale(c, layers)[first:]
        now = stream[pl.ds(starts[c] + first, counts[c] - first), :]
        done = (now * scale * final_gain[...]).astype(jnp.bfloat16)
        out[pl.ds(starts[c] + first - HALO, counts[c] - first), :] = done

    @pl.when(s + 1 < sp_count)
    def _():
        remote(
            tokens.at[pl.ds(rows - HALO, HALO), :], halo, halo_sems.at[0], halo_sems.at[1], {"sp": s + 1}
        ).wait_send()

    def drain_weights(index, carry):
        layer = index // 4
        pair = remote(
            mats[0].at[layer], whole_block(index, s), pair_send.at[index], pair_recv.at[index], {"sp": partner}
        )
        pair.wait_send()
        for by in range(1, chips):
            row_arrival(index, by).wait_send()
            for step in range(1, groups):
                cross_copy(index, by, step).wait_send()
            for step in range(groups):
                relay_copy(index, by, step).wait_send()
        return carry

    lax.fori_loop(0, layers * 4, drain_weights, 0)

    def drain_acts(stage, carry):
        for c in range(2):
            act_each(c, stage, lambda copy: copy.wait_send())
            act_forwards(c, stage, False)
        return carry

    lax.fori_loop(0, layers * 2, drain_acts, 0)

    def drain_squares(index, carry):
        for c in range(2):
            for by in range(1, tp_count):
                sq_copy(c, index, by).wait_send()
        return carry

    lax.fori_loop(0, layers + 1, drain_squares, 0)


def shards(sizes, tokens_in, out_gate, in_gate, value_proj, mix_proj, conv_taps, norm_gains, final_gain):
    groups, sp_count, tp_count, layers, tap_count = sizes
    rows, width = tokens_in.shape
    full = width * tp_count
    chips = sp_count // CORES
    half = rows // 2
    first, second = HALO + half, rows - half
    lanes = lambda n: -(-n // 128) * 128
    dma = pltpu.SemaphoreType.DMA
    near, rounds = max(chips - 1, 1), max((tp_count + 1) // 2 - 1, 1)
    mats = layers * 4
    vmem = pl.BlockSpec(memory_space=pltpu.VMEM)
    hbm = pl.BlockSpec(memory_space=pl.ANY)
    return pl.pallas_call(
        functools.partial(kernel, sizes),
        out_shape=jax.ShapeDtypeStruct((rows, width), jnp.bfloat16),
        in_specs=[vmem] + [hbm] * 4 + [vmem] * 3,
        out_specs=vmem,
        scratch_shapes=[
            pltpu.VMEM((mats, full, width), jnp.bfloat16),
            pltpu.VMEM((2 * layers, first, full), jnp.bfloat16),
            pltpu.VMEM((2 * layers, second, full), jnp.bfloat16),
            pltpu.VMEM((layers + 1, tp_count, 8, lanes(first)), jnp.float32),
            pltpu.VMEM((layers + 1, tp_count, 8, lanes(second)), jnp.float32),
            pltpu.VMEM((HALO + rows, width), jnp.float32),
            pltpu.VMEM((8 + HALO + rows, width), jnp.float32),
            pltpu.VMEM((HALO, width), jnp.bfloat16),
            dma((mats,)),
            dma((2,)),
            dma((mats,)),
            dma((mats,)),
            dma((mats, near)),
            dma((mats, near)),
            dma((mats, near, max(groups - 1, 1))),
            dma((mats, near, max(groups - 1, 1))),
            dma((mats, near, groups)),
            dma((mats, near, groups)),
            dma((2, 2 * layers, 4)),
            dma((2, 2 * layers, tp_count)),
            dma((2, 2 * layers, rounds, 2, 2)),
            dma((2, layers + 1, max(tp_count - 1, 1))),
            dma((2, layers + 1, max(tp_count - 1, 1))),
        ],
        compiler_params=pltpu.CompilerParams(
            collective_id=0, has_side_effects=True, vmem_limit_bytes=VMEM_LIMIT
        ),
    )(tokens_in, in_gate, value_proj, out_gate, mix_proj, conv_taps, norm_gains, final_gain.reshape(1, width))


def solution(mesh):
    in_specs = (
        P(("grp", "sp"), "tp"),
        P(None, "sp", "tp"),
        P(None, "sp", "tp"),
        P(None, "sp", "tp"),
        P(None, "sp", "tp"),
        P(None, None, "tp"),
        P(None, "tp"),
        P("tp"),
    )
    out_specs = P(("grp", "sp"), "tp")

    def body(*args):
        taps = args[5]
        sizes = (mesh.shape["grp"], mesh.shape["sp"], mesh.shape["tp"], taps.shape[0], taps.shape[1])
        return shards(sizes, *args)

    return jax.shard_map(body, mesh=mesh, in_specs=in_specs, out_specs=out_specs, check_vma=False)
```

```python
import functools

import jax
import jax.numpy as jnp
from jax import lax
from jax.experimental import pallas as pl
from jax.experimental.pallas import tpu as pltpu
from jax.sharding import PartitionSpec as P

epsilon = 1e-06
MESH = pl.DeviceIdType.MESH
HALO = 8
CORES = 2
VMEM_LIMIT = 67043328


def kernel(
    sizes,
    tokens,
    in_gate,
    value_proj,
    out_gate,
    mix_proj,
    taps,
    gains,
    final_gain,
    out,
    weights,
    gather_a,
    gather_b,
    squares_a,
    squares_b,
    stream,
    products,
    halo,
    own_sem,
    halo_sems,
    pair_send,
    pair_recv,
    row_send,
    row_recv,
    cross_send,
    cross_recv,
    relay_send,
    relay_recv,
    act_send,
    act_recv,
    act_fwd,
    sq_send,
    sq_recv,
):
    groups, sp_count, tp_count, layers, tap_count = sizes
    rows, width = tokens.shape
    depth = in_gate.shape[1]
    full = depth * sp_count
    part = depth // groups
    chips = sp_count // CORES
    mats = (in_gate, value_proj, out_gate, mix_proj)
    g = lax.axis_index("grp")
    s = lax.axis_index("sp")
    t = lax.axis_index("tp")
    y, core = s // CORES, s % CORES
    partner = y * CORES + (1 - core)
    half = rows // 2
    counts = (HALO + half, rows - half)
    starts = (0, HALO + half)
    gathers = (gather_a, gather_b)
    squares = (squares_a, squares_b)

    def remote(src, dst, send, recv, where):
        return pltpu.make_async_remote_copy(
            src_ref=src, dst_ref=dst, send_sem=send, recv_sem=recv, device_id=where, device_id_type=MESH
        )

    barrier = pltpu.get_barrier_semaphore()
    for axis, me, count in (("tp", t, tp_count), ("sp", s, sp_count), ("grp", g, groups)):
        for by in range(1, count):
            pl.semaphore_signal(barrier, inc=1, device_id={axis: lax.rem(me + by, count)}, device_id_type=MESH)

    for c in range(2):
        for index in range(layers + 1):
            squares[c][index, t] = jnp.zeros(squares[c].shape[2:], jnp.float32)
    products[0:8, :] = jnp.zeros((8, width), jnp.float32)

    @pl.when(s == 0)
    def _():
        halo[...] = jnp.zeros_like(halo)

    pl.semaphore_wait(barrier, tp_count - 1 + sp_count - 1 + groups - 1)

    def block(index, owner, piece):
        return weights.at[index, pl.ds(pl.multiple_of(owner * depth + piece * part, 8), part), :]

    def whole_block(index, owner):
        return weights.at[index, pl.ds(pl.multiple_of(owner * depth, 8), depth), :]

    def own_copy(layer, m):
        index = layer * 4 + m
        return pltpu.make_async_copy(mats[m].at[layer], whole_block(index, s), own_sem.at[index])

    def pair_copy(layer, m, owner):
        index = layer * 4 + m
        return remote(
            mats[m].at[layer], whole_block(index, owner), pair_send.at[index], pair_recv.at[index], {"sp": partner}
        )

    def row_copy(layer, m, by):
        index = layer * 4 + m
        to = lax.rem(y + by, chips) * CORES + core
        return remote(
            mats[m].at[layer, pl.ds(pl.multiple_of(g * part, 8), part), :],
            block(index, s, g),
            row_send.at[index, by - 1],
            row_recv.at[index, by - 1],
            {"sp": to},
        )

    def source(by):
        return lax.rem(y + chips - by, chips) * CORES + core

    def row_arrival(index, by):
        ref = block(index, source(by), g)
        return remote(ref, ref, row_send.at[index, by - 1], row_recv.at[index, by - 1], {"sp": partner})

    def cross_copy(index, by, step):
        ref = block(index, source(by), g)
        return remote(
            ref,
            ref,
            cross_send.at[index, by - 1, step - 1],
            cross_recv.at[index, by - 1, step - 1],
            {"grp": lax.rem(g + step, groups)},
        )

    def cross_arrival(index, by, step):
        ref = block(index, source(by), lax.rem(g + groups - step, groups))
        return remote(
            ref,
            ref,
            cross_send.at[index, by - 1, step - 1],
            cross_recv.at[index, by - 1, step - 1],
            {"grp": lax.rem(g + step, groups)},
        )

    def relay_copy(index, by, step, of_partner=False):
        owner = source(by)
        if of_partner:
            owner = lax.rem(y + chips - by, chips) * CORES + (1 - core)
        ref = block(index, owner, lax.rem(g + groups - step, groups))
        return remote(
            ref, ref, relay_send.at[index, by - 1, step], relay_recv.at[index, by - 1, step], {"sp": partner}
        )

    def serve_rows(index):
        for by in range(1, chips):
            row_arrival(index, by).wait_recv()
            for step in range(1, groups):
                cross_copy(index, by, step).start()
            relay_copy(index, by, 0).start()

    def serve_cross(index):
        for by in range(1, chips):
            for step in range(1, groups):
                cross_arrival(index, by, step).wait_recv()
                relay_copy(index, by, step).start()

    def weights_ready(layer, m):
        index = layer * 4 + m
        own_copy(layer, m).wait()
        pair_copy(layer, m, partner).wait_recv()
        for by in range(1, chips):
            for step in range(groups):
                relay_copy(index, by, step, True).wait_recv()

    def columns(owner):
        return pl.ds(pl.multiple_of(owner * width, 128), width)

    def act_copy(c, stage, owner, to, send):
        ref = gathers[c].at[stage, :, columns(owner)]
        return remote(ref, ref, send, act_recv.at[c, stage, owner], {"tp": to})

    OFFSETS = (2, -2, 1, -1)

    def inside(index):
        return (index >= 0) & (index < tp_count)

    def act_each(c, stage, what):
        for j, by in enumerate(OFFSETS):
            if abs(by) < tp_count:

                @pl.when(inside(t + by))
                def _(j=j, by=by):
                    what(act_copy(c, stage, t, t + by, act_send.at[c, stage, j]))

    def act_forwards(c, stage, start):
        for k in range(1, (tp_count + 1) // 2):
            for side, sign in enumerate((1, -1)):
                origin = t - 2 * k * sign

                @pl.when(inside(origin) & inside(t + sign))
                def _(k=k, side=side, sign=sign, origin=origin):
                    if start:
                        act_copy(c, stage, origin, t + sign, act_fwd.at[c, stage, k - 1, side, 0]).wait_recv()
                    for far in (2, 1):

                        @pl.when(inside(t + sign * far))
                        def _(far=far):
                            copy = act_copy(
                                c, stage, origin, t + sign * far, act_fwd.at[c, stage, k - 1, side, far - 1]
                            )
                            if start:
                                copy.start()
                            else:
                                copy.wait_send()

    def act_finish(c, stage):
        for owner in range(tp_count):
            right = (owner < t) & (lax.rem(t - owner + tp_count * 2, 2) == 0) & (t + 1 < tp_count)
            left = (owner > t) & (lax.rem(owner - t + tp_count * 2, 2) == 0) & (t >= 1)

            @pl.when((owner != t) & jnp.logical_not(right | left))
            def _(owner=owner):
                act_copy(c, stage, owner, t, act_send.at[c, stage, 0]).wait_recv()

    def sq_copy(c, index, by):
        ref = squares[c].at[index, t]
        return remote(
            ref,
            ref,
            sq_send.at[c, index, by - 1],
            sq_recv.at[c, index, by - 1],
            {"tp": lax.rem(t + by, tp_count)},
        )

    def span(c):
        return pl.ds(starts[c], counts[c])

    def send_normed(c, layer):
        now = stream[span(c), :]
        gathers[c][2 * layer, :, columns(t)] = (now * gains[pl.ds(layer, 1), :]).astype(jnp.bfloat16)
        act_each(c, 2 * layer, lambda copy: copy.start())

    def send_squares(c, index):
        now = stream[span(c), :]
        sums = lax.dot_general(
            jnp.ones((8, width), jnp.float32),
            now * now,
            (((1,), (1,)), ((), ())),
            precision=lax.Precision.HIGHEST,
            preferred_element_type=jnp.float32,
        )
        squares[c][index, t, :, 0 : counts[c]] = sums
        for by in range(1, tp_count):
            sq_copy(c, index, by).start()

    def row_scale(c, index):
        for by in range(1, tp_count):
            sq_copy(c, index, by).wait_recv()
        total = squares[c][index, 0]
        for owner in range(1, tp_count):
            total = total + squares[c][index, owner]
        scale = lax.rsqrt(total / full + epsilon)
        return jnp.transpose(scale)[0 : counts[c], 0:1]

    @pl.when(s + 1 < sp_count)
    def _():
        remote(
            tokens.at[pl.ds(rows - HALO, HALO), :], halo, halo_sems.at[0], halo_sems.at[1], {"sp": s + 1}
        ).start()

    for layer in range(1):
        for m in range(3):
            for by in range(1, chips):
                row_copy(layer, m, by).start()
            pair_copy(layer, m, s).start()
            own_copy(layer, m).start()

    stream[HALO:, :] = tokens[...].astype(jnp.float32)
    send_normed(1, 0)

    @pl.when(s > 0)
    def _():
        remote(halo, halo, halo_sems.at[0], halo_sems.at[1], {"sp": partner}).wait_recv()

    stream[0:HALO, :] = halo[...].astype(jnp.float32)
    send_normed(0, 0)
    send_squares(0, 0)
    send_squares(1, 0)

    for index in range(3, layers * 4):
        layer, m = divmod(index, 4)
        for by in range(1, chips):
            row_copy(layer, m, by).start()
        pair_copy(layer, m, s).start()
        own_copy(layer, m).start()

    act_forwards(0, 0, True)
    act_forwards(1, 0, True)
    serve_rows(0)
    serve_rows(1)
    serve_cross(0)
    serve_rows(2)
    serve_cross(1)

    def project(c, layer, before):
        stage = 2 * layer
        act_finish(c, stage)
        seen = gathers[c][stage]
        scale = row_scale(c, layer)

        def projected(m):
            if c == 0:
                if m == 2:
                    pl.when(layer == 0)(lambda: serve_cross(2))
                weights_ready(layer, m)
            product = jnp.dot(seen, weights[layer * 4 + m], preferred_element_type=jnp.float32)
            return (product * scale).astype(jnp.bfloat16)

        ins, values, outs = [projected(m) for m in range(3)]
        made = (ins.astype(jnp.float32) * values.astype(jnp.float32)).astype(jnp.bfloat16)
        products[pl.ds(8 + starts[c], counts[c]), :] = made.astype(jnp.float32)
        total = None
        for k in range(tap_count):
            term = products[pl.ds(8 + starts[c] - (tap_count - 1) + k, counts[c]), :] * taps[layer, pl.ds(k, 1), :]
            total = term if total is None else total + term
        gathers[c][stage + 1, :, columns(t)] = (outs.astype(jnp.float32) * total).astype(jnp.bfloat16)
        before()
        act_each(c, stage + 1, lambda copy: copy.start())

    def mix(c, layer, before):
        stage = 2 * layer + 1
        act_finish(c, stage)
        if c == 0:
            weights_ready(layer, 3)
        stream[span(c), :] += jnp.dot(
            gathers[c][stage], weights[layer * 4 + 3], preferred_element_type=jnp.float32
        )

        before()

        @pl.when(layer + 1 < layers)
        def _():
            send_normed(c, layer + 1)

        send_squares(c, layer + 1)

    def one_layer(layer, carry):
        index = 4 * layer
        more = layer + 1 < layers

        def pass_first():
            @pl.when(more)
            def _():
                act_forwards(0, 2 * layer + 2, True)

        def pass_second():
            @pl.when(layer > 0)
            def _():
                act_forwards(1, 2 * layer, True)

        def serve(first, row_ahead, cross_ahead):
            @pl.when(layer == 0)
            def _():
                for action, at in first:
                    action(at)

            @pl.when((layer > 0) & (index + row_ahead < layers * 4))
            def _():
                serve_rows(index + row_ahead)

            @pl.when((layer > 0) & (index + cross_ahead < layers * 4))
            def _():
                serve_cross(index + cross_ahead)

        project(0, layer, pass_second)
        serve(((serve_rows, 3), (serve_rows, 4)), 5, 3)
        project(1, layer, lambda: act_forwards(0, 2 * layer + 1, True))
        serve(((serve_rows, 5), (serve_cross, 3)), 6, 4)
        mix(0, layer, lambda: act_forwards(1, 2 * layer + 1, True))
        serve(((serve_rows, 6), (serve_cross, 4)), 7, 5)
        mix(1, layer, pass_first)
        serve(((serve_rows, 7), (serve_cross, 5), (serve_rows, 8), (serve_cross, 6)), 8, 6)
        return carry

    lax.fori_loop(0, layers, one_layer, 0)

    for c in range(2):
        first = HALO if c == 0 else 0
        scale = row_scale(c, layers)[first:]
        now = stream[pl.ds(starts[c] + first, counts[c] - first), :]
        done = (now * scale * final_gain[...]).astype(jnp.bfloat16)
        out[pl.ds(starts[c] + first - HALO, counts[c] - first), :] = done

    @pl.when(s + 1 < sp_count)
    def _():
        remote(
            tokens.at[pl.ds(rows - HALO, HALO), :], halo, halo_sems.at[0], halo_sems.at[1], {"sp": s + 1}
        ).wait_send()

    def drain_weights(index, carry):
        layer = index // 4
        pair = remote(
            mats[0].at[layer], whole_block(index, s), pair_send.at[index], pair_recv.at[index], {"sp": partner}
        )
        pair.wait_send()
        for by in range(1, chips):
            row_arrival(index, by).wait_send()
            for step in range(1, groups):
                cross_copy(index, by, step).wait_send()
            for step in range(groups):
                relay_copy(index, by, step).wait_send()
        return carry

    lax.fori_loop(0, layers * 4, drain_weights, 0)

    def drain_acts(stage, carry):
        for c in range(2):
            act_each(c, stage, lambda copy: copy.wait_send())
            act_forwards(c, stage, False)
        return carry

    lax.fori_loop(0, layers * 2, drain_acts, 0)

    def drain_squares(index, carry):
        for c in range(2):
            for by in range(1, tp_count):
                sq_copy(c, index, by).wait_send()
        return carry

    lax.fori_loop(0, layers + 1, drain_squares, 0)


def shards(sizes, tokens_in, out_gate, in_gate, value_proj, mix_proj, conv_taps, norm_gains, final_gain):
    groups, sp_count, tp_count, layers, tap_count = sizes
    rows, width = tokens_in.shape
    full = width * tp_count
    chips = sp_count // CORES
    half = rows // 2
    first, second = HALO + half, rows - half
    lanes = lambda n: -(-n // 128) * 128
    dma = pltpu.SemaphoreType.DMA
    near, rounds = max(chips - 1, 1), max((tp_count + 1) // 2 - 1, 1)
    mats = layers * 4
    vmem = pl.BlockSpec(memory_space=pltpu.VMEM)
    hbm = pl.BlockSpec(memory_space=pl.ANY)
    return pl.pallas_call(
        functools.partial(kernel, sizes),
        out_shape=jax.ShapeDtypeStruct((rows, width), jnp.bfloat16),
        in_specs=[vmem] + [hbm] * 4 + [vmem] * 3,
        out_specs=vmem,
        scratch_shapes=[
            pltpu.VMEM((mats, full, width), jnp.bfloat16),
            pltpu.VMEM((2 * layers, first, full), jnp.bfloat16),
            pltpu.VMEM((2 * layers, second, full), jnp.bfloat16),
            pltpu.VMEM((layers + 1, tp_count, 8, lanes(first)), jnp.float32),
            pltpu.VMEM((layers + 1, tp_count, 8, lanes(second)), jnp.float32),
            pltpu.VMEM((HALO + rows, width), jnp.float32),
            pltpu.VMEM((8 + HALO + rows, width), jnp.float32),
            pltpu.VMEM((HALO, width), jnp.bfloat16),
            dma((mats,)),
            dma((2,)),
            dma((mats,)),
            dma((mats,)),
            dma((mats, near)),
            dma((mats, near)),
            dma((mats, near, max(groups - 1, 1))),
            dma((mats, near, max(groups - 1, 1))),
            dma((mats, near, groups)),
            dma((mats, near, groups)),
            dma((2, 2 * layers, 4)),
            dma((2, 2 * layers, tp_count)),
            dma((2, 2 * layers, rounds, 2, 2)),
            dma((2, layers + 1, max(tp_count - 1, 1))),
            dma((2, layers + 1, max(tp_count - 1, 1))),
        ],
        compiler_params=pltpu.CompilerParams(
            collective_id=0, has_side_effects=True, vmem_limit_bytes=VMEM_LIMIT
        ),
    )(tokens_in, in_gate, value_proj, out_gate, mix_proj, conv_taps, norm_gains, final_gain.reshape(1, width))


def solution(mesh):
    in_specs = (
        P(("grp", "sp"), "tp"),
        P(None, "sp", "tp"),
        P(None, "sp", "tp"),
        P(None, "sp", "tp"),
        P(None, "sp", "tp"),
        P(None, None, "tp"),
        P(None, "tp"),
        P("tp"),
    )
    out_specs = P(("grp", "sp"), "tp")

    def body(*args):
        taps = args[5]
        sizes = (mesh.shape["grp"], mesh.shape["sp"], mesh.shape["tp"], taps.shape[0], taps.shape[1])
        return shards(sizes, *args)

    return jax.shard_map(body, mesh=mesh, in_specs=in_specs, out_specs=out_specs, check_vma=False)
```
